32 devices in a mesh: grp: 2 (over y), ep: 8 (over z, core), tp: 2 (over x).
Axes of the slice: x: 2, y: 2, z: 4, core: 2. Of those that a mesh axis runs over, the one named last changes fastest.
Arguments:
- value_in: bfloat16 [8192, 1024], P(('grp', 'ep'), 'tp'), parts along dimension 0, may hold values from -6 to 6
- gate_in: bfloat16 [8192, 1024], P(('grp', 'ep'), 'tp'), parts along dimension 0, may hold values from -6 to 6
- conv_taps: float32 [31, 1024], P(None, 'tp'), may hold values from -12 to 12
- chan_gain: float32 [1024], replicated, may hold values from 0.1 to 1.9
- out_weight: bfloat16 [1024, 2048], P(None, 'tp'), may hold values from -0.1875 to 0.1875
- second_rows: bfloat16 [2048, 2048], P(('grp', 'ep')), parts along dimension 0, may hold values from -6 to 6
- expert_gain: float32 [2048], replicated, may hold values from 0.1 to 1.9
- routes: int32 [2048, 2], P(('grp', 'ep')), parts along dimension 0, may hold values from 0 to 3, all different within a row; in each aligned block of 128 rows (0 to 127, 128 to 255, ...) at most 96 rows name the same one
- route_weights: float32 [2048, 2], P(('grp', 'ep')), parts along dimension 0, may hold values from 0.1 to 0.9
- gate_w: bfloat16 [8, 2048, 2048], P('ep', None, 'tp'), may hold values from -0.125 to 0.125
- up_w: bfloat16 [8, 2048, 2048], P('ep', None, 'tp'), may hold values from -0.125 to 0.125
- down_w: bfloat16 [8, 2048, 2048], P('ep', 'tp'), may hold values from -0.125 to 0.125
Outputs:
- mixer_rows: bfloat16 [8192, 2048], P(('grp', 'ep'), 'tp'), parts along dimension 0
- routed_rows: bfloat16 [2048, 2048], P(('grp', 'ep'), 'tp'), parts along dimension 0
The draws below stay inside these ranges and needn't reach their ends.
There are 2 independent parts, one for each index of `grp`. The reference program is written for one: setup_inputs(seed, part) draws one part's arguments, and reference() takes and returns one part's arrays. A program takes and returns all parts, laid end to end along the dimension named above; an argument that names none is the same for every part. Nothing has to cross between parts.
Inputs may be any that keep to these rules, and one draw needn't show every extreme that they name: `routes`: in each aligned block of 128 rows (the rows of one index of ep) no expert is named by more than 96 rows, a bound that some block reaches; each row names 2 different experts.
All inputs are finite; a program needn't handle non-finite values.
Results may differ from the reference program's by a relative error of at most 0.017.
Values may be sent and summed in bfloat16 or wider, within the bound.
A program may use at most 64 MiB of HBM per device.

```python
import math
import jax
import jax.numpy as jnp
import numpy as np
from jax import lax

D = 2048
CONV_CH = 1024
TAPS = 31
FF_EXPERT = 4096
TOP = 2
TOK_B = 128
HALF_FF = 2048
EXPERTS = 4
CAP = 96
TOKENS_A = 4096
TOKENS_B = 1024
N_EP = 8
N_TP = 2


def draw_conv_taps(key, part):
    channel = jnp.arange(CONV_CH, dtype=jnp.float32)[None, :] / CONV_CH
    rough = jnp.exp(jax.random.uniform(jax.random.fold_in(key, 7), (1, CONV_CH), jnp.float32, -0.5, 0.5))
    base = jnp.clip(jax.random.normal(jax.random.fold_in(key, 5), (TAPS, CONV_CH), jnp.float32), -4.0, 4.0)
    ramp = jnp.exp(jnp.log(3.0) * channel)
    return base * rough * ramp / math.sqrt(TAPS)


def raised(values, stream_key, source, target, shards_of, factor):
    owner, partner = [(jnp.arange(values.shape[position]) // (values.shape[position] // shards_of)).reshape([-1 if axis == position else 1 for axis in range(values.ndim)]) for position in (source, target)]
    chosen = jax.random.permutation(stream_key, shards_of)[partner]
    strong = (owner == chosen) | (owner == (partner + shards_of // 2) % shards_of)
    return jnp.where(strong, factor * values, values)


def level_of(own_key, dims, split, least, high):
    gain, own = 1.0, jax.random.fold_in(own_key, 6)
    for dim, blocks in split:
        heights = jnp.exp(jax.random.uniform(jax.random.fold_in(own, dim), (blocks,), jnp.float32, least / len(split), high / len(split)))
        gain = gain * jnp.repeat(heights, dims[dim] // blocks).reshape([-1 if axis == dim else 1 for axis in range(len(dims))])
    return gain


def shared_out(key, own, number, rows, number_of, top, reach, skew):
    order = jax.random.permutation(key, number_of)
    heavy_load, usual = load_shares(number_of, rows * top, reach, skew, True), load_shares(number_of, rows * top, reach, skew, False)
    places = jnp.arange(number_of)

    def named(sizes, turn):
        used = int((sizes > 0).sum())
        fixed = max(1, used // 4)
        shifted = fixed + (places - fixed + turn * (used - fixed)) % max(1, number_of - fixed)
        return jnp.zeros((number_of,), jnp.int32).at[order[jnp.where(places < fixed, places, shifted)]].set(jnp.asarray(sizes, jnp.int32))

    sizes = jnp.where(number % 4 == 0, named(heavy_load, number // 4), named(usual, number - number // 4 - 1))
    mixed = jax.random.permutation(jax.random.fold_in(own, 3), number_of)
    donor, taker = mixed[0:number_of // 2 * 2:2], mixed[1:number_of // 2 * 2:2]
    slack = jnp.minimum(sizes[donor] - 1, reach - sizes[taker]) // 2
    slack = jnp.where((donor == order[0]) | (taker == order[0]) | (sizes[taker] == 0), 0, jnp.maximum(slack, 0))
    shifted = jax.random.randint(jax.random.fold_in(own, 4), (number_of // 2,), 0, 1 << 20) % (slack + 1)
    sizes = sizes.at[donor].add(-shifted).at[taker].add(shifted)
    members = jnp.searchsorted(jnp.cumsum(sizes), jnp.arange(rows * top), side="right").astype(jnp.int32)
    table = members.reshape(top, rows).T
    table = table[jax.random.permutation(jax.random.fold_in(own, 1), rows)]
    turn = jax.random.randint(jax.random.fold_in(own, 2), (rows, 1), 0, top)
    return jnp.take_along_axis(table, (jnp.arange(top)[None, :] + turn) % top, axis=1)


def load_shares(amount, total, bound, skew, full):
    loads = [(1 << 20) // math.isqrt(rank ** skew) + 1 for rank in range(1, amount + 1)]
    largest = bound if full else min(bound, max(-(-total // amount), total * loads[0] // sum(loads)))
    least = 1 if total - largest >= amount - 1 else 0
    holding, surplus = [largest] + [least] * (amount - 1), total - largest - least * (amount - 1)
    while surplus > 0:
        candidates = [i for i in range(1, amount) if holding[i] < largest] or [i for i in range(1, amount) if holding[i] < bound]
        whole, left = sum([loads[i] for i in candidates]), surplus
        for i in candidates:
            more = min(bound - holding[i], max(1, left * loads[i] // whole), surplus)
            holding[i] = holding[i] + more
            surplus = surplus - more
    return np.array(holding)


def noise(stream_key, extent, deviation, limit, split=(), kind=jnp.bfloat16):
    values = jax.random.normal(stream_key, extent, jnp.float32) * deviation
    if len(split) > 0:
        values = level_of(stream_key, extent, split, -0.22, 0.18) * values
    return jnp.clip(values, min=-limit, max=limit).astype(kind)


def heavy_noise(own_key, shape, spread, most, pieces, heavy, held_as=jnp.bfloat16):
    entries = spread * jax.random.normal(own_key, shape, jnp.float32)
    if pieces:
        entries = entries * level_of(own_key, shape, pieces, -0.22, 0.18)
    return jnp.clip(raised(entries, jax.random.fold_in(own_key, 3), *heavy), -most, most).astype(held_as)


def setup_inputs(seed: int = 0, part: int = 0) -> dict:
    key_list = jax.random.split(jax.random.key(seed), 13)
    part_keys = jax.random.split(jax.random.fold_in(key_list[12], part), 13)
    value_in = noise(part_keys[0], (TOKENS_A, CONV_CH), 1.0, 6.0, ((0, 8), (1, 2)))
    gate_in = noise(part_keys[1], (TOKENS_A, CONV_CH), 1.0, 6.0, ((0, 8), (1, 2)))
    conv_taps = draw_conv_taps(jax.random.fold_in(key_list[12], 71), part)
    chan_gain = jnp.clip(1.0 + 0.18 * jax.random.normal(key_list[3], (CONV_CH,), jnp.float32), 0.1, 1.9)
    out_weight = noise(key_list[4], (CONV_CH, D), CONV_CH ** -0.5, 0.1875, ((1, 2),))
    second_rows = noise(part_keys[5], (TOKENS_B, D), 1.0, 6.0, ((0, 8),))
    expert_gain = jnp.clip(1.0 + 0.18 * jax.random.normal(key_list[6], (D,), jnp.float32), 0.1, 1.9)
    routes_keys = jax.random.split(jax.random.fold_in(part_keys[7], 1), TOKENS_B // TOK_B)
    routes_turns = jax.random.permutation(jax.random.fold_in(part_keys[7], 3), TOKENS_B // TOK_B)
    routes = jax.vmap(lambda own, number: shared_out(jax.random.fold_in(part_keys[7], 2), own, number, TOK_B, EXPERTS, TOP, CAP, 1))(routes_keys, routes_turns).reshape((TOKENS_B, TOP))
    route_weights = jnp.clip(0.1 + 0.79999997 * jax.random.uniform(part_keys[8], (TOKENS_B, TOP), jnp.float32) ** level_of(part_keys[8], (TOKENS_B, TOP), ((0, 8),), -0.2, 0.2), 0.1, 0.9)
    gate_w = noise(key_list[9], (2 * EXPERTS, D, HALF_FF), D ** -0.5, 0.125, ((0, 8), (2, 2)))
    up_w = noise(key_list[10], (2 * EXPERTS, D, HALF_FF), D ** -0.5, 0.125, ((0, 8), (2, 2)))
    down_w = heavy_noise(key_list[11], (2 * EXPERTS, HALF_FF, D), FF_EXPERT ** -0.5, 0.125, ((0, 8), (1, 2)), (1, 2, 2, 2.0))
    return dict(value_in=value_in, gate_in=gate_in, conv_taps=conv_taps, chan_gain=chan_gain, out_weight=out_weight, second_rows=second_rows, expert_gain=expert_gain, routes=routes, route_weights=route_weights, gate_w=gate_w, up_w=up_w, down_w=down_w)


eps = 1e-06

def expert_values(rows, gate_pair, up_pair, down_pair):
    halves = []
    for half in range(2):
        gate = jnp.dot(rows, gate_pair[half], preferred_element_type=jnp.float32)
        upper = jnp.dot(rows, up_pair[half], preferred_element_type=jnp.float32)
        hidden = (jax.nn.silu(gate) * upper).astype(jnp.bfloat16)
        block = hidden.shape[1] // N_TP
        total = jnp.zeros((rows.shape[0], down_pair.shape[2]), jnp.float32)
        for index in range(N_TP):
            piece = jnp.dot(hidden[:, index * block:(index + 1) * block], down_pair[half, index * block:(index + 1) * block], preferred_element_type=jnp.float32)
            total = total + lax.optimization_barrier(piece.astype(jnp.bfloat16)).astype(jnp.float32)
        halves.append(lax.optimization_barrier(total.astype(jnp.bfloat16)).astype(jnp.float32))
    return (halves[0] + halves[1]).astype(jnp.bfloat16)

def reference(value_in, gate_in, conv_taps, chan_gain, out_weight, second_rows, expert_gain, routes, route_weights, gate_w, up_w, down_w):
    glu = (value_in.astype(jnp.float32) * jax.nn.sigmoid(gate_in.astype(jnp.float32))).astype(jnp.bfloat16)
    length = glu.shape[0]
    padded = jnp.concatenate([jnp.zeros((TAPS - 1, glu.shape[1]), jnp.float32), glu.astype(jnp.float32)], axis=0)
    total = jnp.zeros(glu.shape, jnp.float32)
    for offset in range(TAPS):
        total = total + conv_taps[offset][None, :] * padded[offset:offset + length]
    values = total.astype(jnp.bfloat16).astype(jnp.float32)
    centered = values - lax.optimization_barrier(jnp.mean(values, axis=-1, keepdims=True))
    scaled = centered * lax.rsqrt(lax.optimization_barrier(jnp.mean(centered * centered, axis=-1, keepdims=True)) + eps) * chan_gain
    activated = jax.nn.silu(scaled).astype(jnp.bfloat16)
    mixer_rows = jnp.dot(activated, out_weight, preferred_element_type=jnp.float32).astype(jnp.bfloat16)
    rows = second_rows.astype(jnp.float32)
    normed = (rows * lax.rsqrt(lax.optimization_barrier(jnp.mean(rows * rows, axis=-1, keepdims=True)) + eps) * expert_gain).astype(jnp.bfloat16)
    tokens = normed.shape[0]
    chosen = routes.reshape(-1).astype(jnp.int32)
    hits = (chosen[:, None] == jnp.arange(EXPERTS, dtype=jnp.int32)[None, :]).astype(jnp.int32)
    place = lax.optimization_barrier(jnp.sum((jnp.cumsum(hits, axis=0) - 1) * hits, axis=1)).astype(jnp.int32)
    owner = jnp.repeat(jnp.arange(tokens, dtype=jnp.int32), TOP)
    span = N_EP * CAP
    table = jnp.full((EXPERTS, span), tokens, jnp.int32).at[chosen, place].set(owner)
    padded_rows = jnp.concatenate([normed, jnp.zeros((1, normed.shape[1]), jnp.bfloat16)], axis=0)
    gate_pairs = gate_w.reshape(EXPERTS, 2, gate_w.shape[1], gate_w.shape[2])
    up_pairs = up_w.reshape(EXPERTS, 2, up_w.shape[1], up_w.shape[2])
    down_pairs = down_w.reshape(EXPERTS, 2, down_w.shape[1], down_w.shape[2])

    def one_expert(packed):
        index, gate_pair, up_pair, down_pair = packed
        return expert_values(padded_rows[index], gate_pair, up_pair, down_pair)
    outputs = lax.map(one_expert, (table, gate_pairs, up_pairs, down_pairs))
    flat = outputs.reshape(EXPERTS * span, outputs.shape[2])
    picked = flat[(chosen * span + place).astype(jnp.int32)].astype(jnp.float32)
    weighted = picked * route_weights.reshape(-1)[:, None]
    routed_rows = lax.optimization_barrier(jnp.sum(weighted.reshape(tokens, TOP, weighted.shape[1]), axis=1)).astype(jnp.bfloat16)
    return (mixer_rows, routed_rows)
```

```python
import functools

import jax
import jax.numpy as jnp
from jax import lax
from jax.experimental import pallas as pl
from jax.experimental.pallas import tpu as pltpu
from jax.sharding import PartitionSpec as P

eps = 1e-06
LANES = 128
MESH = pl.DeviceIdType.MESH


def partner_2(value, axis, bit):
    return lax.ppermute(value, axis, [(i, i ^ 1 << bit) for i in range(lax.axis_size(axis))])


def shifted(value, axis, by):
    devices = lax.axis_size(axis)
    pairs = [(i, i + by) for i in range(devices) if 0 <= i + by < devices]
    return lax.ppermute(value, axis, pairs)


def partner(block):
    return partner_2(block, "ep", 0)


def across(block):
    return lax.all_to_all(block, "ep", split_axis=0, concat_axis=0, tiled=True)


def on_device(
    value_in,
    gate_in,
    conv_taps,
    chan_gain,
    out_weight,
    second_rows,
    expert_gain,
    routes,
    route_weights,
    gate_w,
    up_w,
    down_w,
):
    taps = conv_taps.shape[0]
    glu = (value_in.astype(jnp.float32) * jax.nn.sigmoid(gate_in.astype(jnp.float32))).astype(
        jnp.bfloat16
    )
    length = glu.shape[0]
    before = shifted(glu[length - taps + 1 :], "ep", 1)
    padded = jnp.concatenate([before, glu], axis=0).astype(jnp.float32)
    total = jnp.zeros(glu.shape, jnp.float32)
    for offset in range(taps):
        total = total + conv_taps[offset][None, :] * padded[offset : offset + length]
    convolved = total.astype(jnp.bfloat16)
    channels = lax.all_gather(convolved, "tp", axis=1, tiled=True)
    values = channels.astype(jnp.float32)
    centered = values - jnp.mean(values, axis=-1, keepdims=True)
    scaled = (
        centered
        * lax.rsqrt(jnp.mean(centered * centered, axis=-1, keepdims=True) + eps)
        * chan_gain
    )
    activated = jax.nn.silu(scaled).astype(jnp.bfloat16)
    mixer_rows = jnp.dot(activated, out_weight, preferred_element_type=jnp.float32).astype(
        jnp.bfloat16
    )
    n_ep = lax.axis_size("ep")
    experts = n_ep // 2
    tokens = second_rows.shape[0]
    top = routes.shape[1]
    width = second_rows.shape[1]
    capacity = 2 * max(1, min(tokens // 2, 3 * tokens * top // (4 * experts)))
    half_slots = capacity // 2
    rows = second_rows.astype(jnp.float32)
    normed = (
        rows * lax.rsqrt(jnp.mean(rows * rows, axis=-1, keepdims=True) + eps) * expert_gain
    ).astype(jnp.bfloat16)
    chosen = routes.reshape(-1)
    hits = (chosen[:, None] == jnp.arange(experts, dtype=jnp.int32)[None, :]).astype(jnp.int32)
    place = jnp.sum((jnp.cumsum(hits, axis=0) - 1) * hits, axis=1)
    target = (chosen * capacity + place).reshape(tokens, top)
    slots = jnp.arange(experts * capacity, dtype=jnp.int32)
    matches = target[:, :, None] == slots[None, None, :]
    picker = jnp.any(matches, axis=1).astype(jnp.bfloat16)
    outgoing = jnp.dot(picker.T, normed, preferred_element_type=jnp.float32).astype(jnp.bfloat16)
    combiner = jnp.sum(jnp.where(matches, route_weights[:, :, None], 0.0), axis=1)
    upper = lax.axis_index("ep") % 2
    arrived = across(outgoing.reshape(n_ep, half_slots, width))
    other = partner(arrived)
    first = jnp.where(upper == 0, arrived, other)
    second = jnp.where(upper == 0, other, arrived)
    incoming = jnp.concatenate([first, second], axis=1)
    block_rows = incoming.reshape(n_ep * capacity, width)
    gate = jnp.dot(block_rows, gate_w[0], preferred_element_type=jnp.float32)
    lifted = jnp.dot(block_rows, up_w[0], preferred_element_type=jnp.float32)
    hidden = (jax.nn.silu(gate) * lifted).astype(jnp.bfloat16)
    partial_value = jnp.dot(hidden, down_w[0], preferred_element_type=jnp.float32)
    half_sums = lax.psum_scatter(
        partial_value.astype(jnp.bfloat16), "tp", scatter_dimension=1, tiled=True
    )
    columns = half_sums.shape[1]
    half_sums = half_sums.reshape(n_ep, capacity, columns)
    other_sums = partner(half_sums)
    joined = (half_sums.astype(jnp.float32) + other_sums.astype(jnp.float32)).astype(jnp.bfloat16)
    own = lax.dynamic_slice_in_dim(joined, upper * half_slots, half_slots, 1)
    results = across(own).reshape(experts * capacity, columns)
    routed_rows = jnp.dot(
        combiner,
        results.astype(jnp.float32),
        precision=lax.Precision.HIGHEST,
        preferred_element_type=jnp.float32,
    ).astype(jnp.bfloat16)
    return (mixer_rows, routed_rows)


def _xor(value, mask):
    out, bit = value, 1
    while bit <= mask:
        if mask & bit:
            out = out + bit - 2 * bit * lax.rem(lax.div(value, bit), 2)
        bit *= 2
    return out


def _iota(shape, dim):
    return lax.broadcasted_iota(jnp.int32, shape, dim)


def _dot(a, b):
    return jnp.dot(a, b, preferred_element_type=jnp.float32)


def step_kernel(
    chips,
    cap,
    pieces,
    halo,
    value_ref,
    gate_ref,
    taps_ref,
    gain_ref,
    wo_hbm,
    rows_ref,
    egain_ref,
    routes_ref,
    routes_t_ref,
    rw_ref,
    wg_hbm,
    wu_hbm,
    wd_hbm,
    mixer_ref,
    routed_ref,
    wo,
    wg,
    wu,
    wd,
    normed,
    picked,
    block,
    hid,
    part,
    pair_in,
    cross_out,
    cross_in,
    back_out,
    results,
    glu,
    halo_in,
    conv,
    w_sem,
    disp_send,
    disp_recv,
    xf_send,
    xf_recv,
    cf_send,
    cf_recv,
    r1_send,
    r1_recv,
    r2_send,
    r2_recv,
    r3_send,
    r3_recv,
    ag_send,
    ag_recv,
    halo_send,
    halo_recv,
):
    f32, bf16 = jnp.float32, jnp.bfloat16
    ep = lax.axis_index("ep")
    x = lax.axis_index("tp")
    n_ep = 2 * chips
    z, c = lax.div(ep, 2), lax.rem(ep, 2)
    width = block.shape[-1]
    tokens = rows_ref.shape[0]
    length, local = value_ref.shape
    cols = local // LANES
    ntaps = taps_ref.shape[0]
    split_from = max(1, chips // 2)
    peers = [_xor(z, k) for k in range(chips)]

    def dev(zd, cd, xd):
        return {"ep": zd * 2 + cd, "tp": xd}

    def remote(src, dst, send, recv, to):
        return pltpu.make_async_remote_copy(
            src_ref=src, dst_ref=dst, send_sem=send, recv_sem=recv, device_id=to, device_id_type=MESH
        )

    core_peer = dev(z, 1 - c, x)
    plane_peer = dev(z, c, 1 - x)
    after = {"ep": lax.rem(ep + 1, n_ep), "tp": x}
    prior = {"ep": lax.rem(ep + n_ep - 1, n_ep), "tp": x}

    weights = [
        pltpu.make_async_copy(wg_hbm.at[0], wg, w_sem.at[0]),
        pltpu.make_async_copy(wu_hbm.at[0], wu, w_sem.at[1]),
        pltpu.make_async_copy(wd_hbm.at[0], wd, w_sem.at[2]),
        pltpu.make_async_copy(wo_hbm, wo, w_sem.at[3]),
    ]
    for copy in weights:
        copy.start()

    barrier = pltpu.get_barrier_semaphore()
    greeted = [core_peer, plane_peer, after, prior] + [dev(peers[k], c, x) for k in range(1, chips)]
    for to in greeted:
        pl.semaphore_signal(barrier, inc=1, device_id=to, device_id_type=MESH)

    erows = -(-chips // 8) * 8
    r0t, r1t = routes_t_ref[0:1, :], routes_t_ref[1:2, :]
    eid = _iota((erows, tokens), 0)
    hits_t = (r0t == eid) | (r1t == eid)
    earlier_t = (_iota((tokens, tokens), 0) < _iota((tokens, tokens), 1)).astype(f32)
    place_t = _dot(hits_t.astype(f32).astype(bf16), earlier_t.astype(bf16))
    slot_t = jnp.where(hits_t, place_t, -1.0).astype(jnp.int32)

    rows = rows_ref[...].astype(f32)
    scale = lax.rsqrt(jnp.mean(rows * rows, axis=-1, keepdims=True) + eps)
    both = (rows * scale * egain_ref[...]).astype(bf16)
    normed[0] = both[:, :width]
    normed[1] = both[:, width:]

    sends = []
    slots = _iota((cap, tokens), 0)

    def pick(k):
        row = jnp.sum(jnp.where(eid == peers[k], slot_t, 0), axis=0, keepdims=True)
        return (slots == row).astype(f32).astype(bf16)

    for k in range(chips - 1, 0, -1):
        picker = pick(k)
        if k >= split_from:
            picked[k, 0] = _dot(picker, normed[x]).astype(bf16)
        else:
            for h in range(2):
                picked[k, h] = _dot(picker, normed[h]).astype(bf16)
    picker = pick(0)
    for h in range(2):
        block[z, h, c] = _dot(picker, normed[h]).astype(bf16)

    pl.semaphore_wait(barrier, len(greeted))
    for k in range(1, chips):
        to = dev(peers[k], c, x)
        if k >= split_from:
            copies = [
                remote(picked.at[k, 0], block.at[z, x, c], disp_send.at[k, 0], disp_recv.at[z, 0], to)
            ]
        else:
            copies = [
                remote(
                    picked.at[k, h], block.at[z, h, c], disp_send.at[k, h], disp_recv.at[z, h], to
                )
                for h in range(2)
            ]
        for copy in copies:
            copy.start()
        sends.extend(copies)

    def start(copy):
        copy.start()
        sends.append(copy)

    def to_core(k, h, sem):
        zs = peers[k]
        start(
            remote(
                block.at[zs, h, c],
                block.at[zs, h, c],
                cf_send.at[k, sem],
                cf_recv.at[k, sem],
                core_peer,
            )
        )

    def from_core(k, h, sem):
        zs = peers[k]
        remote(
            block.at[zs, h, 1 - c],
            block.at[zs, h, 1 - c],
            cf_send.at[k, sem],
            cf_recv.at[k, sem],
            core_peer,
        ).wait_recv()

    def arrived(k, h, sem):
        zs = peers[k]
        remote(
            block.at[zs, h, c],
            block.at[zs, h, c],
            disp_send.at[k, sem],
            disp_recv.at[zs, sem],
            dev(zs, c, x),
        ).wait_recv()

    def experts(k):
        zs = peers[k]
        a0 = block[zs, 0].reshape(2 * cap, width)
        a1 = block[zs, 1].reshape(2 * cap, width)
        units = hid.shape[1]
        step = min(units, 256)
        for j in range(0, units, step):
            gate = _dot(a0, wg[:width, j : j + step]) + _dot(a1, wg[width:, j : j + step])
            up = _dot(a0, wu[:width, j : j + step]) + _dot(a1, wu[width:, j : j + step])
            hid[:, j : j + step] = (gate * jax.nn.sigmoid(gate) * up).astype(bf16)
        h_all = hid[...]
        for h in range(2):
            for j in range(0, width, step):
                out = _dot(h_all, wd[:, h * width + j : h * width + j + step]).astype(bf16)
                part[k, 0, h, :, j : j + step] = out[:cap]
                part[k, 1, h, :, j : j + step] = out[cap:]
        start(remote(part.at[k, 1 - c], pair_in.at[k], r1_send.at[k], r1_recv.at[k], core_peer))

    def pair_sum(k):
        remote(
            part.at[k, 1 - c], pair_in.at[k], r1_send.at[k], r1_recv.at[k], core_peer
        ).wait_recv()
        total = part[k, c, 1 - x].astype(f32) + pair_in[k, 1 - x].astype(f32)
        cross_out[k] = total.astype(bf16)
        start(remote(cross_out.at[k], cross_in.at[k], r2_send.at[k], r2_recv.at[k], plane_peer))

    def plane_sum(k):
        remote(
            cross_out.at[k], cross_in.at[k], r2_send.at[k], r2_recv.at[k], plane_peer
        ).wait_recv()
        total = part[k, c, x].astype(f32) + pair_in[k, x].astype(f32) + cross_in[k].astype(f32)
        if k == 0:
            results[z] = total.astype(bf16)
        else:
            back_out[k] = total.astype(bf16)
            start(
                remote(
                    back_out.at[k],
                    results.at[z],
                    r3_send.at[k],
                    r3_recv.at[z],
                    dev(peers[k], c, x),
                )
            )

    for h in range(2):
        to_core(0, h, h)

    for i in range(cols):
        part_cols = slice(i * LANES, (i + 1) * LANES)
        gated = value_ref[:, part_cols].astype(f32) * jax.nn.sigmoid(
            gate_ref[:, part_cols].astype(f32)
        )
        glu[i, halo:, :] = gated.astype(bf16).astype(f32)
    start(
        remote(
            glu.at[:, pl.ds(length, halo)], halo_in, halo_send.at[0], halo_recv.at[0], after
        )
    )

    for h in range(2):
        from_core(0, h, h)
    for copy in weights[:3]:
        copy.wait()
    experts(0)

    remote(
        glu.at[:, pl.ds(length, halo)], halo_in, halo_send.at[0], halo_recv.at[0], after
    ).wait_recv()
    glu[:, :halo, :] = jnp.where(ep > 0, halo_in[...], 0.0)
    tile = 64 if length % 64 == 0 else length
    for i in range(cols):

        def conv_tile(r, carry):
            r0 = pl.multiple_of(r * tile, tile)
            total = jnp.zeros((tile, LANES), f32)
            for k in range(ntaps):
                total = (
                    total
                    + taps_ref[k : k + 1, i * LANES : (i + 1) * LANES]
                    * glu[i, pl.ds(r0 + (k + halo - ntaps + 1), tile), :]
                )
            conv[x, pl.ds(r0, tile), i * LANES : (i + 1) * LANES] = total.astype(bf16)
            return carry

        lax.fori_loop(0, length // tile, conv_tile, 0)

    rows_per = length // pieces

    def gather_copy(p):
        own = conv.at[x, pl.ds(p * rows_per, rows_per)]
        return remote(own, own, ag_send.at[p], ag_recv.at[p], plane_peer)

    def gather_some(lo, hi):
        for p in range(lo, hi):
            start(gather_copy(p))

    gather_some(0, pieces // 2)
    for k in range(1, split_from):
        for h in range(2):
            arrived(k, h, h)
            to_core(k, h, h)
    pair_sum(0)
    done = 1
    for k in range(1, split_from):
        for h in range(2):
            from_core(k, h, h)
        experts(k)
    for k in range(split_from, chips):
        arrived(k, x, 0)
        zs = peers[k]
        start(
            remote(block.at[zs, x, c], block.at[zs, x, c], xf_send.at[k], xf_recv.at[k], plane_peer)
        )
        to_core(k, x, 0)
    gather_some(pieces // 2, pieces)
    plane_sum(0)
    for k in range(1, split_from):
        pair_sum(k)
    for k in range(split_from, chips):
        zs = peers[k]
        remote(
            block.at[zs, 1 - x, c], block.at[zs, 1 - x, c], xf_send.at[k], xf_recv.at[k], plane_peer
        ).wait_recv()
        to_core(k, 1 - x, 1)
        from_core(k, x, 0)
        from_core(k, 1 - x, 1)
        experts(k)
        if k > split_from:
            pair_sum(k - 1)
    for k in range(1, split_from):
        plane_sum(k)
    pair_sum(chips - 1)

    weights[3].wait()
    for p in range(pieces):
        other = conv.at[1 - x, pl.ds(p * rows_per, rows_per)]
        remote(other, other, ag_send.at[p], ag_recv.at[p], plane_peer).wait_recv()
        here = slice(p * rows_per, (p + 1) * rows_per)
        lo, hi = conv[0, here, :].astype(f32), conv[1, here, :].astype(f32)
        count = 2 * local
        mean = (
            jnp.sum(lo, axis=-1, keepdims=True) + jnp.sum(hi, axis=-1, keepdims=True)
        ) / count
        lo, hi = lo - mean, hi - mean
        var = (
            jnp.sum(lo * lo, axis=-1, keepdims=True) + jnp.sum(hi * hi, axis=-1, keepdims=True)
        ) / count
        scale = lax.rsqrt(var + eps)
        lo = lo * scale * gain_ref[:, :local]
        hi = hi * scale * gain_ref[:, local:]
        lo = (lo * jax.nn.sigmoid(lo)).astype(bf16)
        hi = (hi * jax.nn.sigmoid(hi)).astype(bf16)
        mixer_ref[here, :] = (_dot(lo, wo[:local, :]) + _dot(hi, wo[local:, :])).astype(bf16)

    for k in range(split_from, chips):
        plane_sum(k)

    lane = _iota((tokens, LANES), 1)
    r0, r1 = routes_ref[:, 0:1], routes_ref[:, 1:2]
    hits = ((r0 == lane) | (r1 == lane)).astype(f32).astype(bf16)
    earlier = (_iota((tokens, tokens), 1) < _iota((tokens, tokens), 0)).astype(f32).astype(bf16)
    place = _dot(earlier, hits)
    all_slots = _iota((tokens, chips * cap), 1)
    comb = jnp.zeros((tokens, chips * cap), f32)
    for j, r in enumerate((r0, r1)):
        at = jnp.sum(jnp.where(lane == r, place, 0.0), axis=1, keepdims=True).astype(jnp.int32)
        comb = comb + jnp.where(all_slots == r * cap + at, rw_ref[:, j : j + 1], 0.0)
    head = comb.astype(bf16)
    tail = (comb - head.astype(f32)).astype(bf16)
    for k in range(1, chips):
        zs = peers[k]
        remote(
            back_out.at[k], results.at[zs], r3_send.at[k], r3_recv.at[zs], dev(zs, c, x)
        ).wait_recv()
    found = results[...].reshape(chips * cap, width)
    routed_ref[...] = (_dot(head, found) + _dot(tail, found)).astype(bf16)
    for copy in sends:
        copy.wait_send()


def one_kernel(
    value_in,
    gate_in,
    conv_taps,
    chan_gain,
    out_weight,
    second_rows,
    expert_gain,
    routes,
    route_weights,
    gate_w,
    up_w,
    down_w,
):
    chips = lax.axis_size("ep") // 2
    tokens, model = second_rows.shape
    top = routes.shape[1]
    width = model // 2
    cap = 2 * max(1, min(tokens // 2, 3 * tokens * top // (4 * chips)))
    length, local = value_in.shape
    units = gate_w.shape[2]
    halo = -(-(conv_taps.shape[0] - 1) // 8) * 8
    pieces = 4
    bf16, f32 = jnp.bfloat16, jnp.float32
    vmem = pl.BlockSpec(memory_space=pltpu.VMEM)
    hbm = pl.BlockSpec(memory_space=pl.ANY)
    dma = pltpu.SemaphoreType.DMA
    scratch = [
        pltpu.VMEM(out_weight.shape, bf16),
        pltpu.VMEM(gate_w.shape[1:], bf16),
        pltpu.VMEM(up_w.shape[1:], bf16),
        pltpu.VMEM(down_w.shape[1:], bf16),
        pltpu.VMEM((2, tokens, width), bf16),
        pltpu.VMEM((chips, 2, cap, width), bf16),
        pltpu.VMEM((chips, 2, 2, cap, width), bf16),
        pltpu.VMEM((2 * cap, units), bf16),
        pltpu.VMEM((chips, 2, 2, cap, width), bf16),
        pltpu.VMEM((chips, 2, cap, width), bf16),
        pltpu.VMEM((chips, cap, width), bf16),
        pltpu.VMEM((chips, cap, width), bf16),
        pltpu.VMEM((chips, cap, width), bf16),
        pltpu.VMEM((chips, cap, width), bf16),
        pltpu.VMEM((local // LANES, halo + length, LANES), f32),
        pltpu.VMEM((local // LANES, halo, LANES), f32),
        pltpu.VMEM((2, length, local), bf16),
        dma((4,)),
        dma((chips, 2)),
        dma((chips, 2)),
        dma((chips,)),
        dma((chips,)),
        dma((chips, 2)),
        dma((chips, 2)),
        dma((chips,)),
        dma((chips,)),
        dma((chips,)),
        dma((chips,)),
        dma((chips,)),
        dma((chips,)),
        dma((pieces,)),
        dma((pieces,)),
        dma((1,)),
        dma((1,)),
    ]
    return pl.pallas_call(
        functools.partial(step_kernel, chips, cap, pieces, halo),
        out_shape=(
            jax.ShapeDtypeStruct((length, out_weight.shape[1]), bf16),
            jax.ShapeDtypeStruct((tokens, width), bf16),
        ),
        in_specs=[vmem] * 4 + [hbm] + [vmem] * 5 + [hbm] * 3,
        out_specs=(vmem, vmem),
        scratch_shapes=scratch,
        compiler_params=pltpu.CompilerParams(
            collective_id=0, has_side_effects=True, vmem_limit_bytes=60 * 1024 * 1024
        ),
    )(
        value_in,
        gate_in,
        conv_taps,
        chan_gain.reshape(1, -1),
        out_weight,
        second_rows,
        expert_gain.reshape(1, -1),
        routes,
        routes.T,
        route_weights,
        gate_w,
        up_w,
        down_w,
    )


def solution(mesh):
    chips = mesh.shape["ep"] // 2
    paired = mesh.shape["tp"] == 2 and chips > 1 and chips & (chips - 1) == 0
    placed = (
        P(("grp", "ep"), "tp"),
        P(("grp", "ep"), "tp"),
        P(None, "tp"),
        P(),
        P(None, "tp"),
        P(("grp", "ep"), None),
        P(),
        P(("grp", "ep"), None),
        P(("grp", "ep"), None),
        P("ep", None, "tp"),
        P("ep", None, "tp"),
        P("ep", "tp", None),
    )
    return jax.shard_map(
        one_kernel if paired else on_device,
        mesh=mesh,
        in_specs=placed,
        out_specs=(P(("grp", "ep"), "tp"), P(("grp", "ep"), "tp")),
        check_vma=False,
    )
```

```python
import functools

import jax
import jax.numpy as jnp
from jax import lax
from jax.experimental import pallas as pl
from jax.experimental.pallas import tpu as pltpu
from jax.sharding import PartitionSpec as P

eps = 1e-06
LANES = 128
MESH = pl.DeviceIdType.MESH


def partner_2(value, axis, bit):
    return lax.ppermute(value, axis, [(i, i ^ 1 << bit) for i in range(lax.axis_size(axis))])


def shifted(value, axis, by):
    devices = lax.axis_size(axis)
    pairs = [(i, i + by) for i in range(devices) if 0 <= i + by < devices]
    return lax.ppermute(value, axis, pairs)


def partner(block):
    return partner_2(block, "ep", 0)


def across(block):
    return lax.all_to_all(block, "ep", split_axis=0, concat_axis=0, tiled=True)


def on_device(
    value_in,
    gate_in,
    conv_taps,
    chan_gain,
    out_weight,
    second_rows,
    expert_gain,
    routes,
    route_weights,
    gate_w,
    up_w,
    down_w,
):
    taps = conv_taps.shape[0]
    glu = (value_in.astype(jnp.float32) * jax.nn.sigmoid(gate_in.astype(jnp.float32))).astype(
        jnp.bfloat16
    )
    length = glu.shape[0]
    before = shifted(glu[length - taps + 1 :], "ep", 1)
    padded = jnp.concatenate([before, glu], axis=0).astype(jnp.float32)
    total = jnp.zeros(glu.shape, jnp.float32)
    for offset in range(taps):
        total = total + conv_taps[offset][None, :] * padded[offset : offset + length]
    convolved = total.astype(jnp.bfloat16)
    channels = lax.all_gather(convolved, "tp", axis=1, tiled=True)
    values = channels.astype(jnp.float32)
    centered = values - jnp.mean(values, axis=-1, keepdims=True)
    scaled = (
        centered
        * lax.rsqrt(jnp.mean(centered * centered, axis=-1, keepdims=True) + eps)
        * chan_gain
    )
    activated = jax.nn.silu(scaled).astype(jnp.bfloat16)
    mixer_rows = jnp.dot(activated, out_weight, preferred_element_type=jnp.float32).astype(
        jnp.bfloat16
    )
    n_ep = lax.axis_size("ep")
    experts = n_ep // 2
    tokens = second_rows.shape[0]
    top = routes.shape[1]
    width = second_rows.shape[1]
    capacity = 2 * max(1, min(tokens // 2, 3 * tokens * top // (4 * experts)))
    half_slots = capacity // 2
    rows = second_rows.astype(jnp.float32)
    normed = (
        rows * lax.rsqrt(jnp.mean(rows * rows, axis=-1, keepdims=True) + eps) * expert_gain
    ).astype(jnp.bfloat16)
    chosen = routes.reshape(-1)
    hits = (chosen[:, None] == jnp.arange(experts, dtype=jnp.int32)[None, :]).astype(jnp.int32)
    place = jnp.sum((jnp.cumsum(hits, axis=0) - 1) * hits, axis=1)
    target = (chosen * capacity + place).reshape(tokens, top)
    slots = jnp.arange(experts * capacity, dtype=jnp.int32)
    matches = target[:, :, None] == slots[None, None, :]
    picker = jnp.any(matches, axis=1).astype(jnp.bfloat16)
    outgoing = jnp.dot(picker.T, normed, preferred_element_type=jnp.float32).astype(jnp.bfloat16)
    combiner = jnp.sum(jnp.where(matches, route_weights[:, :, None], 0.0), axis=1)
    upper = lax.axis_index("ep") % 2
    arrived = across(outgoing.reshape(n_ep, half_slots, width))
    other = partner(arrived)
    first = jnp.where(upper == 0, arrived, other)
    second = jnp.where(upper == 0, other, arrived)
    incoming = jnp.concatenate([first, second], axis=1)
    block_rows = incoming.reshape(n_ep * capacity, width)
    gate = jnp.dot(block_rows, gate_w[0], preferred_element_type=jnp.float32)
    lifted = jnp.dot(block_rows, up_w[0], preferred_element_type=jnp.float32)
    hidden = (jax.nn.silu(gate) * lifted).astype(jnp.bfloat16)
    partial_value = jnp.dot(hidden, down_w[0], preferred_element_type=jnp.float32)
    half_sums = lax.psum_scatter(
        partial_value.astype(jnp.bfloat16), "tp", scatter_dimension=1, tiled=True
    )
    columns = half_sums.shape[1]
    half_sums = half_sums.reshape(n_ep, capacity, columns)
    other_sums = partner(half_sums)
    joined = (half_sums.astype(jnp.float32) + other_sums.astype(jnp.float32)).astype(jnp.bfloat16)
    own = lax.dynamic_slice_in_dim(joined, upper * half_slots, half_slots, 1)
    results = across(own).reshape(experts * capacity, columns)
    routed_rows = jnp.dot(
        combiner,
        results.astype(jnp.float32),
        precision=lax.Precision.HIGHEST,
        preferred_element_type=jnp.float32,
    ).astype(jnp.bfloat16)
    return (mixer_rows, routed_rows)


def _xor(value, mask):
    out, bit = value, 1
    while bit <= mask:
        if mask & bit:
            out = out + bit - 2 * bit * lax.rem(lax.div(value, bit), 2)
        bit *= 2
    return out


def _iota(shape, dim):
    return lax.broadcasted_iota(jnp.int32, shape, dim)


def _dot(a, b):
    return jnp.dot(a, b, preferred_element_type=jnp.float32)


def step_kernel(
    chips,
    cap,
    pieces,
    halo,
    value_ref,
    gate_ref,
    taps_ref,
    gain_ref,
    wo_hbm,
    rows_ref,
    egain_ref,
    routes_t_ref,
    rw_t_ref,
    wg_hbm,
    wu_hbm,
    wd_hbm,
    mixer_ref,
    routed_ref,
    wo,
    wg,
    wu,
    wd,
    normed,
    picked,
    block,
    hid,
    part,
    pair_in,
    cross_out,
    cross_in,
    back_out,
    results,
    glu,
    halo_in,
    conv,
    w_sem,
    disp_send,
    disp_recv,
    xf_send,
    xf_recv,
    cf_send,
    cf_recv,
    r1_send,
    r1_recv,
    r2_send,
    r2_recv,
    r3_send,
    r3_recv,
    ag_send,
    ag_recv,
    halo_send,
    halo_recv,
):
    f32, bf16 = jnp.float32, jnp.bfloat16
    ep = lax.axis_index("ep")
    x = lax.axis_index("tp")
    n_ep = 2 * chips
    z, c = lax.div(ep, 2), lax.rem(ep, 2)
    width = block.shape[-1]
    tokens = rows_ref.shape[0]
    length, local = value_ref.shape
    cols = local // LANES
    ntaps = taps_ref.shape[0]
    split_from = max(1, chips // 2)
    peers = [_xor(z, k) for k in range(chips)]

    def dev(zd, cd, xd):
        return {"ep": zd * 2 + cd, "tp": xd}

    def remote(src, dst, send, recv, to):
        return pltpu.make_async_remote_copy(
            src_ref=src, dst_ref=dst, send_sem=send, recv_sem=recv, device_id=to, device_id_type=MESH
        )

    core_peer = dev(z, 1 - c, x)
    plane_peer = dev(z, c, 1 - x)
    after = {"ep": lax.rem(ep + 1, n_ep), "tp": x}
    prior = {"ep": lax.rem(ep + n_ep - 1, n_ep), "tp": x}

    weights = [
        pltpu.make_async_copy(wg_hbm.at[0], wg, w_sem.at[0]),
        pltpu.make_async_copy(wu_hbm.at[0], wu, w_sem.at[1]),
        pltpu.make_async_copy(wd_hbm.at[0], wd, w_sem.at[2]),
        pltpu.make_async_copy(wo_hbm, wo, w_sem.at[3]),
    ]
    for copy in weights:
        copy.start()

    barrier = pltpu.get_barrier_semaphore()
    greeted = [core_peer, plane_peer, after, prior] + [dev(peers[k], c, x) for k in range(1, chips)]
    for to in greeted:
        pl.semaphore_signal(barrier, inc=1, device_id=to, device_id_type=MESH)

    erows = -(-chips // 8) * 8
    r0t, r1t = routes_t_ref[0:1, :], routes_t_ref[1:2, :]
    eid = _iota((erows, tokens), 0)
    hits_t = (r0t == eid) | (r1t == eid)
    earlier_t = (_iota((tokens, tokens), 0) < _iota((tokens, tokens), 1)).astype(f32)
    place_t = _dot(hits_t.astype(f32).astype(bf16), earlier_t.astype(bf16))
    slot_t = jnp.where(hits_t, place_t, -1.0).astype(jnp.int32)

    rows = rows_ref[...].astype(f32)
    scale = lax.rsqrt(jnp.mean(rows * rows, axis=-1, keepdims=True) + eps)
    both = (rows * scale * egain_ref[...]).astype(bf16)
    normed[0] = both[:, :width]
    normed[1] = both[:, width:]

    sends = []
    slots = _iota((cap, tokens), 0)

    def pick(k):
        row = jnp.sum(jnp.where(eid == peers[k], slot_t, 0), axis=0, keepdims=True)
        return (slots == row).astype(f32).astype(bf16)

    for k in range(chips - 1, 0, -1):
        picker = pick(k)
        if k >= split_from:
            picked[k, 0] = _dot(picker, normed[x]).astype(bf16)
        else:
            for h in range(2):
                picked[k, h] = _dot(picker, normed[h]).astype(bf16)
    picker = pick(0)
    for h in range(2):
        block[z, h, c] = _dot(picker, normed[h]).astype(bf16)

    pl.semaphore_wait(barrier, len(greeted))
    subs = 2 if cap % 32 == 0 else 1
    far = list(range(split_from, chips))
    near = list(range(1, split_from))

    def sub(s):
        return pl.ds(s * (cap // subs), cap // subs)

    for k in far + near:
        to = dev(peers[k], c, x)
        if k >= split_from:
            copies = [
                remote(
                    picked.at[k, 0, sub(s)],
                    block.at[z, x, c, sub(s)],
                    disp_send.at[k, s],
                    disp_recv.at[z, s],
                    to,
                )
                for s in range(subs)
            ]
        else:
            copies = [
                remote(
                    picked.at[k, h], block.at[z, h, c], disp_send.at[k, h], disp_recv.at[z, h], to
                )
                for h in range(2)
            ]
        for copy in copies:
            copy.start()
        sends.extend(copies)

    def start(copy):
        copy.start()
        sends.append(copy)

    whole = pl.ds(0, cap)

    def to_core(k, h, sem, rows_of=whole):
        here = block.at[peers[k], h, c, rows_of]
        start(remote(here, here, cf_send.at[k, sem], cf_recv.at[k, sem], core_peer))

    def from_core(k, h, sem, rows_of=whole):
        here = block.at[peers[k], h, 1 - c, rows_of]
        remote(here, here, cf_send.at[k, sem], cf_recv.at[k, sem], core_peer).wait_recv()

    def arrived(k, h, sem, rows_of=whole):
        here = block.at[peers[k], h, c, rows_of]
        remote(
            here, here, disp_send.at[k, sem], disp_recv.at[peers[k], sem], dev(peers[k], c, x)
        ).wait_recv()

    def experts(k):
        zs = peers[k]
        a0 = block[zs, 0].reshape(2 * cap, width)
        a1 = block[zs, 1].reshape(2 * cap, width)
        units = hid.shape[1]
        step = min(units, 256)
        for j in range(0, units, step):
            gate = _dot(a0, wg[:width, j : j + step]) + _dot(a1, wg[width:, j : j + step])
            up = _dot(a0, wu[:width, j : j + step]) + _dot(a1, wu[width:, j : j + step])
            hid[:, j : j + step] = (gate * jax.nn.sigmoid(gate) * up).astype(bf16)
        h_all = hid[...]
        for h in range(2):
            for j in range(0, width, step):
                out = _dot(h_all, wd[:, h * width + j : h * width + j + step]).astype(bf16)
                part[k, 0, h, :, j : j + step] = out[:cap]
                part[k, 1, h, :, j : j + step] = out[cap:]
        start(remote(part.at[k, 1 - c], pair_in.at[k], r1_send.at[k], r1_recv.at[k], core_peer))

    def pair_sum(k):
        remote(
            part.at[k, 1 - c], pair_in.at[k], r1_send.at[k], r1_recv.at[k], core_peer
        ).wait_recv()
        total = part[k, c, 1 - x].astype(f32) + pair_in[k, 1 - x].astype(f32)
        cross_out[k] = total.astype(bf16)
        start(remote(cross_out.at[k], cross_in.at[k], r2_send.at[k], r2_recv.at[k], plane_peer))

    def plane_sum(k):
        remote(
            cross_out.at[k], cross_in.at[k], r2_send.at[k], r2_recv.at[k], plane_peer
        ).wait_recv()
        total = part[k, c, x].astype(f32) + pair_in[k, x].astype(f32) + cross_in[k].astype(f32)
        if k == 0:
            results[z] = total.astype(bf16)
        else:
            back_out[k] = total.astype(bf16)
            start(
                remote(
                    back_out.at[k],
                    results.at[z],
                    r3_send.at[k],
                    r3_recv.at[z],
                    dev(peers[k], c, x),
                )
            )

    for h in range(2):
        to_core(0, h, h)

    for i in range(cols):
        part_cols = slice(i * LANES, (i + 1) * LANES)
        gated = value_ref[:, part_cols].astype(f32) * jax.nn.sigmoid(
            gate_ref[:, part_cols].astype(f32)
        )
        glu[i, halo:, :] = gated.astype(bf16).astype(f32)
    start(
        remote(
            glu.at[:, pl.ds(length, halo)], halo_in, halo_send.at[0], halo_recv.at[0], after
        )
    )

    for h in range(2):
        from_core(0, h, h)
    for copy in weights[:3]:
        copy.wait()
    experts(0)

    remote(
        glu.at[:, pl.ds(length, halo)], halo_in, halo_send.at[0], halo_recv.at[0], after
    ).wait_recv()
    glu[:, :halo, :] = jnp.where(ep > 0, halo_in[...], 0.0)
    tile = 64 if length % 64 == 0 else length
    for i in range(cols):

        def conv_tile(r, carry):
            r0 = pl.multiple_of(r * tile, tile)
            total = jnp.zeros((tile, LANES), f32)
            for k in range(ntaps):
                total = (
                    total
                    + taps_ref[k : k + 1, i * LANES : (i + 1) * LANES]
                    * glu[i, pl.ds(r0 + (k + halo - ntaps + 1), tile), :]
                )
            conv[x, pl.ds(r0, tile), i * LANES : (i + 1) * LANES] = total.astype(bf16)
            return carry

        lax.fori_loop(0, length // tile, conv_tile, 0)

    rows_per = length // pieces

    def gather_copy(p):
        own = conv.at[x, pl.ds(p * rows_per, rows_per)]
        return remote(own, own, ag_send.at[p], ag_recv.at[p], plane_peer)

    def gather_some(lo, hi):
        for p in range(lo, hi):
            start(gather_copy(p))

    gather_some(0, 1)
    for k in far:
        for s in range(subs):
            arrived(k, x, s, sub(s))
            here = block.at[peers[k], x, c, sub(s)]
            start(remote(here, here, xf_send.at[k, s], xf_recv.at[k, s], plane_peer))
            to_core(k, x, s, sub(s))
    pair_sum(0)
    for k in near:
        for h in range(2):
            arrived(k, h, h)
            to_core(k, h, h)
    for k in near:
        for h in range(2):
            from_core(k, h, h)
        experts(k)
    for k in far:
        for s in range(subs):
            here = block.at[peers[k], 1 - x, c, sub(s)]
            remote(here, here, xf_send.at[k, s], xf_recv.at[k, s], plane_peer).wait_recv()
            to_core(k, 1 - x, subs + s, sub(s))
        if k == far[0]:
            for q in near:
                pair_sum(q)
        for s in range(subs):
            from_core(k, x, s, sub(s))
            from_core(k, 1 - x, subs + s, sub(s))
        experts(k)
        if k > far[0]:
            plane_sum(k - 1)
        pair_sum(k)
    gather_some(1, pieces)
    for k in near:
        plane_sum(k)
    plane_sum(chips - 1)
    plane_sum(0)

    weights[3].wait()
    for p in range(pieces):
        other = conv.at[1 - x, pl.ds(p * rows_per, rows_per)]
        remote(other, other, ag_send.at[p], ag_recv.at[p], plane_peer).wait_recv()
        here = slice(p * rows_per, (p + 1) * rows_per)
        lo, hi = conv[0, here, :].astype(f32), conv[1, here, :].astype(f32)
        count = 2 * local
        mean = (
            jnp.sum(lo, axis=-1, keepdims=True) + jnp.sum(hi, axis=-1, keepdims=True)
        ) / count
        lo, hi = lo - mean, hi - mean
        var = (
            jnp.sum(lo * lo, axis=-1, keepdims=True) + jnp.sum(hi * hi, axis=-1, keepdims=True)
        ) / count
        scale = lax.rsqrt(var + eps)
        lo = lo * scale * gain_ref[:, :local]
        hi = hi * scale * gain_ref[:, local:]
        lo = (lo * jax.nn.sigmoid(lo)).astype(bf16)
        hi = (hi * jax.nn.sigmoid(hi)).astype(bf16)
        mixer_ref[here, :] = (_dot(lo, wo[:local, :]) + _dot(hi, wo[local:, :])).astype(bf16)

    lane = _iota((tokens, LANES), 1)
    index = _iota((8, tokens), 0)
    rows_named = jnp.where(index == 0, r0t, 0).astype(f32) + jnp.where(index == 1, r1t, 0).astype(f32)
    for j in range(2):
        rows_named = rows_named + jnp.where(index == 2 + j, rw_t_ref[j : j + 1, :], 0.0)
    named = jnp.transpose(rows_named)
    r0, r1 = (named[:, j : j + 1].astype(jnp.int32) for j in range(2))
    hits = ((r0 == lane) | (r1 == lane)).astype(f32).astype(bf16)
    earlier = (_iota((tokens, tokens), 1) < _iota((tokens, tokens), 0)).astype(f32).astype(bf16)
    place = _dot(earlier, hits)
    all_slots = _iota((tokens, chips * cap), 1)
    comb = jnp.zeros((tokens, chips * cap), f32)
    for j, r in enumerate((r0, r1)):
        at = jnp.sum(jnp.where(lane == r, place, 0.0), axis=1, keepdims=True).astype(jnp.int32)
        comb = comb + jnp.where(all_slots == r * cap + at, named[:, 2 + j : 3 + j], 0.0)
    head = comb.astype(bf16)
    tail = (comb - head.astype(f32)).astype(bf16)
    for k in range(1, chips):
        zs = peers[k]
        remote(
            back_out.at[k], results.at[zs], r3_send.at[k], r3_recv.at[zs], dev(zs, c, x)
        ).wait_recv()
    found = results[...].reshape(chips * cap, width)
    routed_ref[...] = (_dot(head, found) + _dot(tail, found)).astype(bf16)
    for copy in sends:
        copy.wait_send()


def one_kernel(
    value_in,
    gate_in,
    conv_taps,
    chan_gain,
    out_weight,
    second_rows,
    expert_gain,
    routes,
    route_weights,
    gate_w,
    up_w,
    down_w,
):
    chips = lax.axis_size("ep") // 2
    tokens, model = second_rows.shape
    top = routes.shape[1]
    width = model // 2
    cap = 2 * max(1, min(tokens // 2, 3 * tokens * top // (4 * chips)))
    length, local = value_in.shape
    units = gate_w.shape[2]
    halo = -(-(conv_taps.shape[0] - 1) // 8) * 8
    pieces = 4
    bf16, f32 = jnp.bfloat16, jnp.float32
    vmem = pl.BlockSpec(memory_space=pltpu.VMEM)
    hbm = pl.BlockSpec(memory_space=pl.ANY)
    dma = pltpu.SemaphoreType.DMA
    scratch = [
        pltpu.VMEM(out_weight.shape, bf16),
        pltpu.VMEM(gate_w.shape[1:], bf16),
        pltpu.VMEM(up_w.shape[1:], bf16),
        pltpu.VMEM(down_w.shape[1:], bf16),
        pltpu.VMEM((2, tokens, width), bf16),
        pltpu.VMEM((chips, 2, cap, width), bf16),
        pltpu.VMEM((chips, 2, 2, cap, width), bf16),
        pltpu.VMEM((2 * cap, units), bf16),
        pltpu.VMEM((chips, 2, 2, cap, width), bf16),
        pltpu.VMEM((chips, 2, cap, width), bf16),
        pltpu.VMEM((chips, cap, width), bf16),
        pltpu.VMEM((chips, cap, width), bf16),
        pltpu.VMEM((chips, cap, width), bf16),
        pltpu.VMEM((chips, cap, width), bf16),
        pltpu.VMEM((local // LANES, halo + length, LANES), f32),
        pltpu.VMEM((local // LANES, halo, LANES), f32),
        pltpu.VMEM((2, length, local), bf16),
        dma((4,)),
        dma((chips, 2)),
        dma((chips, 2)),
        dma((chips, 2)),
        dma((chips, 2)),
        dma((chips, 4)),
        dma((chips, 4)),
        dma((chips,)),
        dma((chips,)),
        dma((chips,)),
        dma((chips,)),
        dma((chips,)),
        dma((chips,)),
        dma((pieces,)),
        dma((pieces,)),
        dma((1,)),
        dma((1,)),
    ]
    return pl.pallas_call(
        functools.partial(step_kernel, chips, cap, pieces, halo),
        out_shape=(
            jax.ShapeDtypeStruct((length, out_weight.shape[1]), bf16),
            jax.ShapeDtypeStruct((tokens, width), bf16),
        ),
        in_specs=[vmem] * 4 + [hbm] + [vmem] * 4 + [hbm] * 3,
        out_specs=(vmem, vmem),
        scratch_shapes=scratch,
        compiler_params=pltpu.CompilerParams(
            collective_id=0, has_side_effects=True, vmem_limit_bytes=60 * 1024 * 1024
        ),
    )(
        value_in,
        gate_in,
        conv_taps,
        chan_gain.reshape(1, -1),
        out_weight,
        second_rows,
        expert_gain.reshape(1, -1),
        routes.T,
        route_weights.T,
        gate_w,
        up_w,
        down_w,
    )


def solution(mesh):
    chips = mesh.shape["ep"] // 2
    paired = mesh.shape["tp"] == 2 and chips > 1 and chips & (chips - 1) == 0
    placed = (
        P(("grp", "ep"), "tp"),
        P(("grp", "ep"), "tp"),
        P(None, "tp"),
        P(),
        P(None, "tp"),
        P(("grp", "ep"), None),
        P(),
        P(("grp", "ep"), None),
        P(("grp", "ep"), None),
        P("ep", None, "tp"),
        P("ep", None, "tp"),
        P("ep", "tp", None),
    )
    return jax.shard_map(
        one_kernel if paired else on_device,
        mesh=mesh,
        in_specs=placed,
        out_specs=(P(("grp", "ep"), "tp"), P(("grp", "ep"), "tp")),
        check_vma=False,
    )
```
